512 devices in a mesh: sp: 32 (over z, core), tp: 16 (over y, x).
Axes of the slice: x: 4, y: 4, z: 16, core: 2. Of those that a mesh axis runs over, the one named last changes fastest.
Arguments:
- residual_in: bfloat16 [8192, 2048], P(('sp', 'tp')), may hold values from -6 to 6
- query_a: bfloat16 [8192, 1024], P('sp', 'tp'), may hold values from -12 to 12
- key_a: bfloat16 [8192, 1024], P('sp', 'tp'), may hold values from -12 to 12
- value_a: bfloat16 [8192, 1024], P('sp', 'tp'), may hold values from -6 to 6
- query_b: bfloat16 [8192, 2048], P('sp', 'tp'), may hold values from -12 to 12
- key_b: bfloat16 [8192, 2048], P('sp', 'tp'), may hold values from -12 to 12
- value_b: bfloat16 [8192, 2048], P('sp', 'tp'), may hold values from -6 to 6
- cum_gates: float32 [8192, 2, 16], P('sp', None, 'tp'), may hold values from -985.04 to 0, as said below
- out_a: bfloat16 [1024, 2048], P('tp'), may hold values from -0.1875 to 0.1875
- out_b: bfloat16 [2048, 2048], P('tp'), may hold values from -0.125 to 0.125
- post_gain: bfloat16 [2048], replicated, may hold values from 0.099609375 to 1.8984375
- pre_gain: bfloat16 [2048], replicated, may hold values from 0.099609375 to 1.8984375
- expert_ids: int32 [8192, 2], P('sp'), may hold values from 0 to 31, all different within a row; in each aligned block of 256 rows (0 to 255, 256 to 511, ...) at most 20 rows name the same one
- expert_weights: float32 [8192, 2], P('sp'), may hold values from 0.2 to 1
- w_gate: bfloat16 [32, 2048, 4096], P('sp', None, 'tp'), may hold values from -0.125 to 0.125
- w_up: bfloat16 [32, 2048, 4096], P('sp', None, 'tp'), may hold values from -0.125 to 0.125
- w_down: bfloat16 [32, 4096, 2048], P('sp', 'tp'), may hold values from -0.09375 to 0.09375
Outputs:
- layer_out: bfloat16 [8192, 2048], P(('sp', 'tp'))
The draws below stay inside these ranges and needn't reach their ends.
Inputs may be any that keep to these rules, and one draw needn't show every extreme that they name: `expert_ids`: in each aligned block of 256 positions no expert is named by more than 20 routes, a bound that some block reaches; a token's experts differ. `cum_gates`: never rises along the positions.
All inputs are finite; a program needn't handle non-finite values.
Results may differ from the reference program's by a relative error of at most 0.015.
Values may be sent and summed in bfloat16 or wider, within the bound.
A program may use at most 64 MiB of HBM per device.

```python
import math
import jax
import jax.numpy as jnp
import numpy as np
from jax import lax

D = 2048
HEADS = 16
DA = 64
DB = 128
FF = 4096
TOP = 2
TOK_DEV = 256
SEQUENCE_TOKENS = 8192
EXPERTS = 32
FF_DEV = 256
SLOTS = 20
N_SP = 32
N_TP = 16


def paired_rows(key, width):
    query_key, keys_key = jax.random.split(key, 2)
    shape = (SEQUENCE_TOKENS, HEADS * width)
    query = jnp.clip(jax.random.normal(query_key, shape, jnp.float32), -4.0, 4.0)
    key_rows = jnp.clip(jax.random.normal(keys_key, shape, jnp.float32), -4.0, 4.0)
    return (query, key_rows)


def value_matrix(key, width):
    noise_key, offset_key = jax.random.split(key, 2)
    shape = (SEQUENCE_TOKENS, HEADS * width)
    noise = jnp.clip(jax.random.normal(noise_key, shape, jnp.float32), -4.0, 4.0) * 0.7
    offsets = jnp.clip(jax.random.normal(offset_key, (N_SP, HEADS * width), jnp.float32), -3.0, 3.0)
    return noise + jnp.repeat(offsets, TOK_DEV, axis=0)


def draw_query_a(key, part):
    return paired_rows(jax.random.fold_in(key, 101), DA)[0].astype(jnp.bfloat16)


def draw_key_a(key, part):
    return paired_rows(jax.random.fold_in(key, 101), DA)[1].astype(jnp.bfloat16)


def draw_query_b(key, part):
    return paired_rows(jax.random.fold_in(key, 202), DB)[0].astype(jnp.bfloat16)


def draw_key_b(key, part):
    return paired_rows(jax.random.fold_in(key, 202), DB)[1].astype(jnp.bfloat16)


def draw_value_a(key, part):
    return value_matrix(jax.random.fold_in(key, 303), DA).astype(jnp.bfloat16)


def draw_value_b(key, part):
    return value_matrix(jax.random.fold_in(key, 404), DB).astype(jnp.bfloat16)


def draw_cum_gates(key, part):
    item_count = 2 * HEADS
    key_rows = jax.random.split(jax.random.fold_in(key, 505), 7)
    fast = jax.random.permutation(key_rows[0], item_count) < HEADS
    fast_span = jnp.exp(jax.random.uniform(key_rows[1], (item_count,), jnp.float32, math.log(30.0), math.log(100.0)))
    slow_total = jax.random.uniform(key_rows[2], (item_count,), jnp.float32, 0.4, 0.8)
    rate = jnp.where(fast, 1.0 / fast_span, slow_total / SEQUENCE_TOKENS)
    factor = jnp.exp(jax.random.uniform(key_rows[3], (N_SP,), jnp.float32, math.log(0.5), math.log(2.0)))
    rough = jax.random.uniform(key_rows[4], (SEQUENCE_TOKENS, item_count), jnp.float32, 0.3, 1.7)
    step_total = -rate[None, :] * jnp.repeat(factor, TOK_DEV)[:, None] * rough
    spike_position = jax.random.randint(key_rows[5], (2,), 0, SEQUENCE_TOKENS)
    spike_length = jnp.log(jax.random.uniform(key_rows[6], (2, item_count), jnp.float32, 0.5, 0.8))
    step_total = step_total.at[spike_position].add(spike_length)
    return jnp.cumsum(step_total, axis=0).reshape(SEQUENCE_TOKENS, 2, HEADS)


def levels(rng, extent, cuts, low, largest):
    level, own = 1.0, jax.random.fold_in(rng, 6)
    for dim, blocks in cuts:
        draws = jnp.exp(jax.random.uniform(jax.random.fold_in(own, dim), (blocks,), jnp.float32, low / len(cuts), largest / len(cuts)))
        level = level * jnp.repeat(draws, extent[dim] // blocks).reshape([-1 if axis == dim else 1 for axis in range(len(extent))])
    return level


def deal_out(own_key, own, number, rows, number_of, top, most, lean):
    ranking = jax.random.permutation(own_key, number_of)
    packed, common = portions_of(number_of, rows * top, most, lean, True), portions_of(number_of, rows * top, most, lean, False)
    places = jnp.arange(number_of)

    def named(sizes, rotation):
        used = int((sizes > 0).sum())
        fixed = max(1, used // 4)
        shifted = fixed + (places - fixed + rotation * (used - fixed)) % max(1, number_of - fixed)
        return jnp.zeros((number_of,), jnp.int32).at[ranking[jnp.where(places < fixed, places, shifted)]].set(jnp.asarray(sizes, jnp.int32))

    sizes = jnp.where(number % 4 == 0, named(packed, number // 4), named(common, number - number // 4 - 1))
    mixed = jax.random.permutation(jax.random.fold_in(own, 3), number_of)
    giver, receiver = mixed[0:number_of // 2 * 2:2], mixed[1:number_of // 2 * 2:2]
    slack = jnp.minimum(sizes[giver] - 1, most - sizes[receiver]) // 2
    slack = jnp.where((giver == ranking[0]) | (receiver == ranking[0]) | (sizes[receiver] == 0), 0, jnp.maximum(slack, 0))
    shifted = jax.random.randint(jax.random.fold_in(own, 4), (number_of // 2,), 0, 1 << 20) % (slack + 1)
    sizes = sizes.at[giver].add(-shifted).at[receiver].add(shifted)
    labels = jnp.searchsorted(jnp.cumsum(sizes), jnp.arange(rows * top), side="right").astype(jnp.int32)
    grid = labels.reshape(top, rows).T
    grid = grid[jax.random.permutation(jax.random.fold_in(own, 1), rows)]
    rotation = jax.random.randint(jax.random.fold_in(own, 2), (rows, 1), 0, top)
    return jnp.take_along_axis(grid, (jnp.arange(top)[None, :] + rotation) % top, axis=1)


def portions_of(count, total, most, skew, full):
    weights = [(1 << 20) // math.isqrt(standing ** skew) + 1 for standing in range(1, count + 1)]
    largest = most if full else min(most, max(-(-total // count), total * weights[0] // sum(weights)))
    least = 1 if total - largest >= count - 1 else 0
    holding, rest = [largest] + [least] * (count - 1), total - largest - least * (count - 1)
    while rest > 0:
        free = [i for i in range(1, count) if holding[i] < largest] or [i for i in range(1, count) if holding[i] < most]
        whole, remaining = sum([weights[i] for i in free]), rest
        for i in free:
            addition = min(most - holding[i], max(1, remaining * weights[i] // whole), rest)
            holding[i] = holding[i] + addition
            rest = rest - addition
    return np.array(holding)


def normal_values(own_key, shape, spread, reach, cuts=(), kind=jnp.bfloat16):
    values = spread * jax.random.normal(own_key, shape, jnp.float32)
    if cuts:
        values = values * levels(own_key, shape, cuts, -0.22, 0.18)
    return jnp.clip(values, -reach, reach).astype(kind)


def setup_inputs(seed: int = 0) -> dict:
    seeds = jax.random.split(jax.random.key(seed), 18)
    residual_in = normal_values(seeds[0], (SEQUENCE_TOKENS, D), 1.0, 6.0, ((0, 512),))
    query_a = draw_query_a(jax.random.fold_in(seeds[17], 71), 0)
    key_a = draw_key_a(jax.random.fold_in(seeds[17], 71), 0)
    value_a = draw_value_a(jax.random.fold_in(seeds[17], 71), 0)
    query_b = draw_query_b(jax.random.fold_in(seeds[17], 71), 0)
    key_b = draw_key_b(jax.random.fold_in(seeds[17], 71), 0)
    value_b = draw_value_b(jax.random.fold_in(seeds[17], 71), 0)
    cum_gates = draw_cum_gates(jax.random.fold_in(seeds[17], 71), 0)
    out_a = normal_values(seeds[8], (HEADS * DA, D), (HEADS * DA) ** -0.5, 0.1875, ((0, 16),))
    out_b = normal_values(seeds[9], (HEADS * DB, D), (HEADS * DB) ** -0.5, 0.125, ((0, 16),))
    post_gain = jnp.clip(1.0 + 0.18 * jax.random.normal(seeds[10], (D,), jnp.float32), 0.099609375, 1.8984375).astype(jnp.bfloat16)
    pre_gain = jnp.clip(1.0 + 0.18 * jax.random.normal(seeds[11], (D,), jnp.float32), 0.099609375, 1.8984375).astype(jnp.bfloat16)
    expert_ids_keys = jax.random.split(jax.random.fold_in(seeds[12], 1), SEQUENCE_TOKENS // TOK_DEV)
    expert_ids_turns = jax.random.permutation(jax.random.fold_in(seeds[12], 3), SEQUENCE_TOKENS // TOK_DEV)
    expert_ids = jax.vmap(lambda own, number: deal_out(jax.random.fold_in(seeds[12], 2), own, number, TOK_DEV, EXPERTS, TOP, SLOTS, 2))(expert_ids_keys, expert_ids_turns).reshape((SEQUENCE_TOKENS, TOP))
    expert_weights = jnp.clip(jnp.exp(math.log(1.0) - 1.609438 * jax.random.uniform(seeds[13], (SEQUENCE_TOKENS, TOP), jnp.float32) ** levels(seeds[13], (SEQUENCE_TOKENS, TOP), ((0, 32),), -0.2, 0.2)), 0.2, 1.0)
    w_gate = normal_values(seeds[14], (EXPERTS, D, FF), D ** -0.5, 0.125, ((0, 32), (2, 16)))
    w_up = normal_values(seeds[15], (EXPERTS, D, FF), D ** -0.5, 0.125, ((0, 32), (2, 16)))
    w_down = normal_values(seeds[16], (EXPERTS, FF, D), FF ** -0.5, 0.09375, ((0, 32), (1, 16)))
    return dict(residual_in=residual_in, query_a=query_a, key_a=key_a, value_a=value_a, query_b=query_b, key_b=key_b, value_b=value_b, cum_gates=cum_gates, out_a=out_a, out_b=out_b, post_gain=post_gain, pre_gain=pre_gain, expert_ids=expert_ids, expert_weights=expert_weights, w_gate=w_gate, w_up=w_up, w_down=w_down)


eps_norm = 1e-06
big_neg = -1e+30

def group_attention(query, key_rows, values, gates, width):
    total_rows = query.shape[0]
    heads = gates.shape[1]
    query_heads = query.reshape(total_rows, heads, width).transpose(1, 0, 2)
    key_heads = key_rows.reshape(total_rows, heads, width).transpose(1, 0, 2)
    value_heads = values.reshape(total_rows, heads, width).transpose(1, 0, 2)
    gate_heads = gates.T
    block = min(512, total_rows)
    blocks = total_rows // block
    key_pos = jnp.arange(total_rows, dtype=jnp.int32)

    def one_head(pieces):
        head_query, head_key, head_value, head_gate = pieces

        def one_block(index):
            start = (index * block).astype(jnp.int32)
            block_query = lax.dynamic_slice_in_dim(head_query, start, block, 0)
            block_gate = lax.dynamic_slice_in_dim(head_gate, start, block, 0)
            score = jnp.dot(block_query, head_key.T, preferred_element_type=jnp.float32) * width ** (-0.5)
            score = score + block_gate[:, None] - head_gate[None, :]
            position = start + jnp.arange(block, dtype=jnp.int32)
            mask = key_pos[None, :] <= position[:, None]
            highest = lax.optimization_barrier(jnp.max(jnp.where(mask, score, big_neg), axis=1, keepdims=True))
            expo = jnp.exp(jnp.where(mask, score - highest, big_neg))
            total = lax.optimization_barrier(jnp.sum(expo, axis=1, keepdims=True))
            mixed = jnp.dot(expo.astype(jnp.bfloat16), head_value, preferred_element_type=jnp.float32)
            return (mixed / total).astype(jnp.bfloat16)
        return lax.map(one_block, jnp.arange(blocks, dtype=jnp.int32)).reshape(total_rows, width)
    result = lax.map(one_head, (query_heads, key_heads, value_heads, gate_heads))
    return result.transpose(1, 0, 2).reshape(total_rows, heads * width)

def head_projection(attn_a, attn_b, out_a, out_b):
    rows_a = out_a.shape[0] // N_TP
    rows_b = out_b.shape[0] // N_TP

    def add_block(index, accum):
        part_a = lax.dynamic_slice_in_dim(attn_a, index * rows_a, rows_a, 1)
        weight_a = lax.dynamic_slice_in_dim(out_a, index * rows_a, rows_a, 0)
        part_b = lax.dynamic_slice_in_dim(attn_b, index * rows_b, rows_b, 1)
        weight_b = lax.dynamic_slice_in_dim(out_b, index * rows_b, rows_b, 0)
        term = jnp.dot(part_a, weight_a, preferred_element_type=jnp.float32) + jnp.dot(part_b, weight_b, preferred_element_type=jnp.float32)
        rounded = lax.optimization_barrier(term.astype(jnp.bfloat16))
        return accum + rounded.astype(jnp.float32)
    start = jnp.zeros((attn_a.shape[0], out_a.shape[1]), jnp.float32)
    return lax.fori_loop(0, N_TP, add_block, start).astype(jnp.bfloat16)

def rms_scale(values, gain):
    return values * lax.rsqrt(lax.optimization_barrier(jnp.mean(values * values, axis=-1, keepdims=True)) + eps_norm) * gain

def reference(residual_in, query_a, key_a, value_a, query_b, key_b, value_b, cum_gates, out_a, out_b, post_gain, pre_gain, expert_ids, expert_weights, w_gate, w_up, w_down):
    attn_a = group_attention(query_a, key_a, value_a, cum_gates[:, 0, :], DA)
    attn_b = group_attention(query_b, key_b, value_b, cum_gates[:, 1, :], DB)
    proj = head_projection(attn_a, attn_b, out_a, out_b)
    post = rms_scale(proj.astype(jnp.float32), post_gain.astype(jnp.float32))
    mid_stream = (residual_in.astype(jnp.float32) + post).astype(jnp.bfloat16)
    normed = rms_scale(mid_stream.astype(jnp.float32), pre_gain.astype(jnp.float32)).astype(jnp.bfloat16)
    block_ids = expert_ids.reshape(N_SP, TOK_DEV * TOP)
    onehot = (block_ids[:, :, None] == jnp.arange(EXPERTS, dtype=jnp.int32)[None, None, :]).astype(jnp.int32)
    rank = lax.optimization_barrier(jnp.sum((jnp.cumsum(onehot, axis=1) - onehot) * onehot, axis=2))
    block_index = jnp.arange(N_SP, dtype=jnp.int32)[:, None]
    target = block_ids * (N_SP * SLOTS) + block_index * SLOTS + rank
    owner = block_index * TOK_DEV + jnp.arange(TOK_DEV * TOP, dtype=jnp.int32)[None, :] // TOP
    table = jnp.full((EXPERTS * N_SP * SLOTS,), -1, jnp.int32).at[target.reshape(-1)].set(owner.reshape(-1))
    table = table.reshape(EXPERTS, N_SP * SLOTS)

    def run_expert(pieces):
        row_index, gate_weight, up_weight, down_weight = pieces
        live = row_index >= 0
        rows = jnp.where(live[:, None], normed[jnp.maximum(row_index, 0)], jnp.zeros((), jnp.bfloat16))
        gate = jnp.dot(rows, gate_weight, preferred_element_type=jnp.float32)
        upward = jnp.dot(rows, up_weight, preferred_element_type=jnp.float32)
        hidden = (jax.nn.silu(gate) * upward).astype(jnp.bfloat16)
        parts = jnp.einsum('rjf,jfd->rjd', hidden.reshape(-1, N_TP, FF_DEV).astype(jnp.float32), down_weight.reshape(N_TP, FF_DEV, D).astype(jnp.float32))
        rounded = lax.optimization_barrier(parts.astype(jnp.bfloat16))
        return lax.optimization_barrier(jnp.sum(rounded.astype(jnp.float32), axis=1)).astype(jnp.bfloat16)
    expert_out = lax.map(run_expert, (table, w_gate, w_up, w_down))
    slot_of = rank.reshape(SEQUENCE_TOKENS, TOP)
    token_block = (jnp.arange(SEQUENCE_TOKENS, dtype=jnp.int32) // TOK_DEV)[:, None]
    picked = expert_out[expert_ids, token_block * SLOTS + slot_of]
    mixture = lax.optimization_barrier(jnp.sum(expert_weights[:, :, None] * picked.astype(jnp.float32), axis=1))
    return (mid_stream.astype(jnp.float32) + mixture).astype(jnp.bfloat16)
```

```python
import functools

import jax
import jax.numpy as jnp
from jax import lax
from jax.experimental import pallas as pl
from jax.experimental.pallas import tpu as pltpu
from jax.sharding import PartitionSpec as P

eps_norm = 1e-06
big_neg = -1e30
log2e = 1.4426950408889634
MESH = pl.DeviceIdType.MESH
VM = pl.BlockSpec(memory_space=pltpu.VMEM)
f32, bf16 = jnp.float32, jnp.bfloat16


def nt_dot(a, b):
    return lax.dot_general(a, b, (((1,), (1,)), ((), ())), preferred_element_type=f32)


def attend_kernel(
    group, q_a, k_a, v_a, q_b, k_b, v_b, gates, w_a, w_b, part,
    kv_a, kv_k, kv_v, kv_g, qa, high_a, tot_a, acc_a, high_b, tot_b, acc_b,
    ring_send, ring_recv, mate_send, mate_recv,
):
    rows = q_b.shape[0]
    da = q_a.shape[0]
    db = q_b.shape[1]
    chips = group // 2
    half = chips // 2
    me = lax.axis_index("sp")
    z, core = me // 2, lax.rem(me, 2)
    right, left = lax.rem(me + 2, group), lax.rem(me + group - 2, group)
    mate = me + 1 - 2 * core
    barrier = pltpu.get_barrier_semaphore()
    for peer in (right, left, mate):
        pl.semaphore_signal(barrier, inc=1, device_id={"sp": peer}, device_id_type=MESH)
    kv_a[me, :da, :] = k_a[...]
    kv_a[me, da:, :] = v_a[...]
    kv_k[me] = k_b[...]
    kv_v[me] = v_b[...]
    kv_g[me] = gates[...]
    qa[...] = q_a[...].astype(f32).T.astype(bf16)
    for high, tot, acc in ((high_a, tot_a, acc_a), (high_b, tot_b, acc_b)):
        high[...] = jnp.full_like(high, big_neg)
        tot[...] = jnp.zeros_like(tot)
        acc[...] = jnp.zeros_like(acc)
    pl.semaphore_wait(barrier, 3)

    bufs = (kv_g, kv_a, kv_k, kv_v)

    def hop(way, k, i, blk):
        return pltpu.make_async_remote_copy(
            src_ref=bufs[i].at[blk], dst_ref=bufs[i].at[blk],
            send_sem=ring_send.at[way, k, i], recv_sem=ring_recv.at[way, k, i],
            device_id={"sp": (right, left)[way]}, device_id_type=MESH,
        )

    def across(way, k, i, blk):
        return pltpu.make_async_remote_copy(
            src_ref=bufs[i].at[blk], dst_ref=bufs[i].at[blk],
            send_sem=mate_send.at[way, k, i], recv_sem=mate_recv.at[way, k, i],
            device_id={"sp": mate}, device_id_type=MESH,
        )

    def block_of(way, k, base):
        shift = (group - 2 * k) if way == 0 else 2 * k
        return lax.rem(base + shift, group)

    for i in range(4):
        hop(0, 1, i, me).start()
        hop(1, 1, i, me).start()
        across(0, 0, i, me).start()

    def update(blocks, mask, query, keys, values, scale, which, high, tot, acc):
        scores = []
        for blk in blocks:
            s = keys(query, blk) * (scale * log2e) - kv_g[blk, which] * log2e
            if mask is not None:
                s = jnp.where(mask, s, big_neg)
            scores.append(s)
        top = jnp.max(functools.reduce(jnp.maximum, scores), axis=1, keepdims=True)
        old = high[...]
        new = jnp.maximum(old, top)
        fade = jnp.exp2(old - new)
        high[...] = new
        weights = [jnp.exp2(s - new) for s in scores]
        tot[...] = tot[...] * fade + jnp.sum(functools.reduce(jnp.add, weights), axis=1, keepdims=True)
        mixed = functools.reduce(jnp.add, [values(w.astype(bf16), blk) for w, blk in zip(weights, blocks)])
        acc[...] = acc[...] * fade + mixed

    def fold(blocks, mask=None):
        update(
            blocks, mask, qa[...],
            lambda q, blk: jnp.dot(q, kv_a[blk, :da, :], preferred_element_type=f32),
            lambda w, blk: nt_dot(w, kv_a[blk, da:, :]),
            da ** -0.5, 0, high_a, tot_a, acc_a,
        )
        update(
            blocks, mask, q_b[...],
            lambda q, blk: nt_dot(q, kv_k[blk]),
            lambda w, blk: jnp.dot(w, kv_v[blk], preferred_element_type=f32),
            db ** -0.5, 1, high_b, tot_b, acc_b,
        )

    row = lax.broadcasted_iota(jnp.int32, (rows, rows), 0)
    col = lax.broadcasted_iota(jnp.int32, (rows, rows), 1)
    fold([me], col <= row)
    for i in range(4):
        across(0, 0, i, mate).wait_recv()

    @pl.when(core == 1)
    def _():
        fold([mate])

    def needed(way, k):
        return (z >= k) if way == 0 else (z + k >= chips)

    def unit(way, k):
        for i in range(4):
            across(way, k, i, block_of(way, k, mate)).wait_recv()

        @pl.when(needed(way, k))
        def _():
            fold([block_of(way, k, me), block_of(way, k, mate)])

    def take(way, k, i, onward):
        blk = block_of(way, k, me)
        hop(way, k, i, blk).wait_recv()
        if onward is True:
            hop(way, k + 1, i, blk).start()
        elif onward is not None:
            @pl.when(onward)
            def _():
                hop(way, k + 1, i, blk).start()
        across(way, k, i, blk).start()

    last_way = (0, 0, 0, 1)

    def step(k, carry):
        for i in range(2):
            for way in range(2):
                take(way, k, i, True if last_way[i] == way else k < half - 1)

        @pl.when(k > 1)
        def _():
            unit(0, k - 1)

        for way in range(2):
            take(way, k, 2, True if last_way[2] == way else k < half - 1)

        @pl.when(k > 1)
        def _():
            unit(1, k - 1)

        for way in range(2):
            take(way, k, 3, True if last_way[3] == way else k < half - 1)
        return carry

    lax.fori_loop(1, half, step, 0)
    unit(0, half - 1)
    unit(1, half - 1)
    for i in range(4):
        way = last_way[i]
        blk = block_of(way, half, me)
        hop(way, half, i, blk).wait_recv()
        across(0, half, i, blk).start()
    unit(0, half)

    out_a = (acc_a[...] / tot_a[...]).astype(bf16)
    out_b = (acc_b[...] / tot_b[...]).astype(bf16)
    wide = min(512, part.shape[1])
    for at in range(0, part.shape[1], wide):
        cols = slice(at, at + wide)
        part[:, cols] = (
            jnp.dot(out_a, w_a[:, cols], preferred_element_type=f32)
            + jnp.dot(out_b, w_b[:, cols], preferred_element_type=f32)
        ).astype(bf16)

    def drain(k, carry):
        for i in range(4):
            for way in range(2):
                hop(way, k, i, me).wait_send()
                across(way, k, i, me).wait_send()
        return carry

    lax.fori_loop(1, half, drain, 0)
    for i in range(4):
        hop(last_way[i], half, i, me).wait_send()
        across(0, half, i, me).wait_send()
        across(0, 0, i, me).wait_send()


def attend(query_a, key_a, value_a, query_b, key_b, value_b, cum_gates, out_a, out_b):
    rows, da = query_a.shape
    db = query_b.shape[1]
    group = lax.axis_size("sp")
    half = group // 4
    return pl.pallas_call(
        functools.partial(attend_kernel, group),
        out_shape=jax.ShapeDtypeStruct((rows, out_a.shape[1]), bf16),
        in_specs=[VM] * 9,
        out_specs=VM,
        scratch_shapes=[
            pltpu.VMEM((group, 2 * da, rows), bf16),
            pltpu.VMEM((group, rows, db), bf16),
            pltpu.VMEM((group, rows, db), bf16),
            pltpu.VMEM((group, 2, 1, rows), f32),
            pltpu.VMEM((rows, da), bf16),
            pltpu.VMEM((rows, 1), f32),
            pltpu.VMEM((rows, 1), f32),
            pltpu.VMEM((rows, da), f32),
            pltpu.VMEM((rows, 1), f32),
            pltpu.VMEM((rows, 1), f32),
            pltpu.VMEM((rows, db), f32),
            pltpu.SemaphoreType.DMA((2, half + 1, 4)),
            pltpu.SemaphoreType.DMA((2, half + 1, 4)),
            pltpu.SemaphoreType.DMA((2, half + 1, 4)),
            pltpu.SemaphoreType.DMA((2, half + 1, 4)),
        ],
        compiler_params=pltpu.CompilerParams(collective_id=1, has_side_effects=True),
        name="attend",
    )(
        query_a.T, key_a.T, value_a.T, query_b, key_b, value_b,
        cum_gates.transpose(1, 2, 0), out_a, out_b,
    )


def joined_along(blocks, dim):
    dims = list(blocks.shape[1:])
    dims[dim] *= blocks.shape[0]
    return jnp.moveaxis(blocks, 0, dim).reshape(dims)


def from_everyone(array, axis):
    copies = jnp.broadcast_to(array, (lax.axis_size(axis), *array.shape))
    return lax.all_to_all(copies, axis, split_axis=0, concat_axis=0, tiled=True)


def gathered_copies(array, axis, dim):
    return joined_along(from_everyone(array, axis), dim)


def side_by_side(arrays, axis, dim, along):
    ends, at = ([], 0)
    for a in arrays[:-1]:
        at += a.shape[along]
        ends.append(at)
    both = jnp.concatenate(arrays, axis=along)
    return tuple(jnp.split(lax.all_gather(both, axis, axis=dim, tiled=True), ends, axis=along))


def split_up(array, dim, devices):
    before, after = (array.shape[:dim], array.shape[dim + 1 :])
    return jnp.moveaxis(array.reshape(*before, devices, -1, *after), dim, 0)


def summed_on_arrival(array, axis, dim):
    blocks = split_up(array, dim, lax.axis_size(axis))
    arrived = lax.all_to_all(blocks, axis, split_axis=0, concat_axis=0, tiled=True)
    return arrived.astype(jnp.float32).sum(axis=0)


def rms_scale(values, gain):
    return values * lax.rsqrt(jnp.mean(values * values, axis=-1, keepdims=True) + eps_norm) * gain


def empty_state(item_count, heads, width):
    return (
        jnp.full((heads, item_count), big_neg, jnp.float32),
        jnp.zeros((heads, item_count), jnp.float32),
        jnp.zeros((heads, item_count, width), jnp.float32),
    )


def update_state(state, query, key_rows, values, query_gate, key_gate, mask, width):
    highest, total, accum = state
    score = jnp.einsum(
        "rhd,khd->hrk", query, key_rows, preferred_element_type=jnp.float32
    ) * width ** (-0.5)
    score = score + query_gate.T[:, :, None] - key_gate.T[:, None, :]
    new_high = jnp.maximum(highest, jnp.max(jnp.where(mask[None], score, big_neg), axis=2))
    expo = jnp.exp(jnp.where(mask[None], score - new_high[:, :, None], big_neg))
    total = jnp.sum(expo, axis=2)
    accum = jnp.einsum(
        "hrk,khd->hrd", expo.astype(jnp.bfloat16), values, preferred_element_type=jnp.float32
    )
    return (new_high, total, accum)


def finish(state):
    highest, total, accum = state
    heads, item_count, width = accum.shape
    result = accum / total[:, :, None]
    return result.transpose(1, 0, 2).reshape(item_count, heads * width).astype(jnp.bfloat16)


def per_device(
    residual_in,
    query_a,
    key_a,
    value_a,
    query_b,
    key_b,
    value_b,
    cum_gates,
    out_a,
    out_b,
    post_gain,
    pre_gain,
    expert_ids,
    expert_weights,
    w_gate,
    w_up,
    w_down,
):
    rows = query_a.shape[0]
    heads = cum_gates.shape[2]
    width_a = query_a.shape[1] // heads
    width_b = query_b.shape[1] // heads
    group_size = lax.axis_size("sp")
    narrow = lax.axis_size("tp")
    here = lax.axis_index("sp")
    offset = here * rows
    part = attend(
        query_a, key_a, value_a, query_b, key_b, value_b, cum_gates, out_a, out_b
    )
    proj = summed_on_arrival(
        part,
        "tp",
        0,
    ).astype(jnp.bfloat16)
    post = rms_scale(proj.astype(jnp.float32), post_gain.astype(jnp.float32))
    mid_stream = (residual_in.astype(jnp.float32) + post).astype(jnp.bfloat16)
    normed = rms_scale(mid_stream.astype(jnp.float32), pre_gain.astype(jnp.float32)).astype(
        jnp.bfloat16
    )
    selected_count = expert_ids.shape[1]
    columns = normed.shape[1] // narrow
    slots = rows * selected_count * 5 // (4 * group_size)
    flat_experts = expert_ids.reshape(-1)
    onehot = (flat_experts[:, None] == jnp.arange(group_size, dtype=jnp.int32)[None, :]).astype(
        jnp.int32
    )
    rank = jnp.sum((jnp.cumsum(onehot, axis=0) - onehot) * onehot, axis=1)
    target = flat_experts * slots + rank
    owner = jnp.arange(rows * selected_count, dtype=jnp.int32) // selected_count
    table = jnp.full((group_size * slots,), -1, jnp.int32).at[target].set(owner)
    live = table >= 0
    source = jnp.maximum(table, 0)
    weighting = jnp.sum(
        expert_weights[:, :, None]
        * (
            target.reshape(rows, selected_count)[:, :, None]
            == jnp.arange(group_size * slots, dtype=jnp.int32)[None, None, :]
        ),
        axis=1,
    )
    column_rows = lax.all_to_all(normed, "tp", split_axis=1, concat_axis=0, tiled=True)
    outgoing = jnp.where(live[:, None], column_rows[source], jnp.zeros((), jnp.bfloat16))
    outgoing = outgoing.reshape(group_size, slots, columns)
    arrived = lax.all_to_all(outgoing, "sp", split_axis=0, concat_axis=0, tiled=True)
    flat = arrived.reshape(-1, columns)
    piece = gathered_copies(flat, "tp", 1)
    gate_rows = w_gate[0]
    up_rows = w_up[0]
    gate = jnp.dot(piece, gate_rows, preferred_element_type=jnp.float32)
    upward = jnp.dot(piece, up_rows, preferred_element_type=jnp.float32)
    hidden_rows = (jax.nn.silu(gate) * upward).astype(jnp.bfloat16)
    hidden = hidden_rows.reshape(arrived.shape[0], arrived.shape[1], -1)
    flat_hidden = hidden.reshape(-1, hidden.shape[2])
    down_cols = w_down[0]
    summed = summed_on_arrival(
        lax.dot_general(
            down_cols, flat_hidden, (((0,), (1,)), ((), ())), preferred_element_type=jnp.float32
        ).astype(jnp.bfloat16),
        "tp",
        0,
    )
    returned = lax.all_to_all(
        summed.astype(jnp.bfloat16).reshape(columns, group_size, slots),
        "sp",
        split_axis=1,
        concat_axis=1,
        tiled=True,
    )
    mixture_cols = jnp.einsum(
        "te,ce->tc", weighting, returned.reshape(columns, group_size * slots).astype(jnp.float32)
    )
    mixture = lax.all_to_all(
        mixture_cols.astype(jnp.bfloat16), "tp", split_axis=0, concat_axis=1, tiled=True
    ).astype(mixture_cols.dtype)
    return (mid_stream.astype(jnp.float32) + mixture).astype(jnp.bfloat16)


def solution(mesh):
    placed = (
        P(("sp", "tp"), None),
        P("sp", "tp"),
        P("sp", "tp"),
        P("sp", "tp"),
        P("sp", "tp"),
        P("sp", "tp"),
        P("sp", "tp"),
        P("sp", None, "tp"),
        P("tp", None),
        P("tp", None),
        P(),
        P(),
        P("sp", None),
        P("sp", None),
        P("sp", None, "tp"),
        P("sp", None, "tp"),
        P("sp", "tp", None),
    )
    return jax.shard_map(
        per_device, mesh=mesh, in_specs=placed, out_specs=P(("sp", "tp"), None), check_vma=False
    )
```
